32 devices in a mesh: ep: 8 (over z, x), tp: 4 (over y, core).
Axes of the slice: x: 2, y: 2, z: 4, core: 2. Of those that a mesh axis runs over, the one named last changes fastest.
Arguments:
- residual: bfloat16 [1024, 2048], P('ep', 'tp'), may hold values from -61 to 61
- in_gain: float32 [2048], replicated, may hold values from 0.1 to 1.9
- in_weight: bfloat16 [2048, 1024], P(None, 'tp'), may hold values from -0.125 to 0.125
- state: float32 [2, 1024, 4096], P(None, 'ep', 'tp'), may hold values from -3 to 3
- decay_rate: float32 [64, 64], P('tp'), may hold values from 0.1 to 1
- frequency: float32 [64, 64], P('tp'), may hold values from 0 to 200
- log_step: float32 [64], P('tp'), may hold values from -3 to -0.7
- in_coef: float32 [2, 64, 64, 16], P(None, 'tp'), may hold values from -1 to 1
- out_coef: float32 [2, 64, 16, 64], P(None, 'tp'), may hold values from -0.75 to 0.75
- skip_gain: float32 [1024], P('tp'), may hold values from -3 to 3
- out_weight: bfloat16 [1024, 2048], replicated, may hold values from -0.1875 to 0.1875
- mid_gain: float32 [2048], replicated, may hold values from 0.1 to 1.9
- gate_vector: bfloat16 [2048], replicated, may hold values from -0.125 to 0.125
- routes: int32 [1024, 4], P('ep'), may hold values from 0 to 31, all different within a row; in each aligned block of 128 rows (0 to 127, 128 to 255, ...) at most 32 rows name the same one
- route_weight: float32 [1024, 4], P('ep'), may hold values from 0.1 to 1
- expert_gate: bfloat16 [32, 2048, 512], P(('ep', 'tp')), may hold values from -0.125 to 0.125
- expert_up: bfloat16 [32, 2048, 512], P(('ep', 'tp')), may hold values from -0.125 to 0.125
- expert_down: bfloat16 [32, 512, 2048], P(('ep', 'tp')), may hold values from -0.25 to 0.25
- shared_gate: bfloat16 [2048, 4096], P(None, 'ep'), may hold values from -0.125 to 0.125
- shared_up: bfloat16 [2048, 4096], P(None, 'ep'), may hold values from -0.125 to 0.125
- shared_down: bfloat16 [4096, 2048], P('ep'), may hold values from -0.09375 to 0.09375
Outputs:
- layer_out: bfloat16 [1024, 2048], P(('ep', 'tp'))
- new_state: float32 [2, 1024, 4096], P(None, 'ep', 'tp')
The draws below stay inside these ranges and needn't reach their ends.
Inputs may be any that keep to these rules, and one draw needn't show every extreme that they name: `routes`: each row names 4 different experts. Among the rows of one index of ep no expert is named more than 32 times, a bound that some block reaches.
All inputs are finite; a program needn't handle non-finite values.
Results may differ from the reference program's by a relative error of at most 0.0085.
Values may be sent and summed in bfloat16 or wider, within the bound.
A program may use at most 128 MiB of HBM per device.

```python
import math
import jax
import jax.numpy as jnp
import numpy as np
from jax import lax

D = 2048
SW = 1024
GROUP_CH = 16
STATE = 64
GROUPS = 64
GS = 4096
FF = 512
SFF = 4096
TOP = 4
SEQ_DEV = 128
SEQS = 1024
EXPERTS = 32
CAP = 32
N_EP = 8


def draw_residual(key, part):
    first_key, second_key = jax.random.split(jax.random.fold_in(key, 11))
    columns = jnp.arange(D, dtype=jnp.float32)
    col_scale = 10.0 ** (columns / D - 0.5)
    row_scale = 10.0 ** jax.random.uniform(second_key, (SEQS, 1), jnp.float32, -0.5, 0.5)
    base_draw = jnp.clip(jax.random.normal(first_key, (SEQS, D), jnp.float32), -6.0, 6.0)
    return (base_draw * col_scale * row_scale).astype(jnp.bfloat16)


def levels(stream_key, shape, cuts, low, high):
    def one(axis_at, blocks):
        draws = jax.random.uniform(jax.random.fold_in(jax.random.fold_in(stream_key, 6), axis_at), (blocks,), jnp.float32, low / len(cuts), high / len(cuts))
        return jnp.repeat(jnp.exp(draws), shape[axis_at] // blocks).reshape((-1,) + (1,) * (len(shape) - axis_at - 1))

    gain = one(*cuts[0])
    for cut in cuts[1:]:
        gain = gain * one(*cut)
    return gain


def deal_out(stream_key, own, number, rows, number_of, top, most, slope):
    order = jax.random.permutation(stream_key, number_of)
    crowded, common = load_shares(number_of, rows * top, most, slope, True), load_shares(number_of, rows * top, most, slope, False)
    places = jnp.arange(number_of)

    def named(sizes, offset_by):
        used = int((sizes > 0).sum())
        fixed = max(1, used // 4)
        moved = fixed + (places - fixed + offset_by * (used - fixed)) % max(1, number_of - fixed)
        return jnp.zeros((number_of,), jnp.int32).at[order[jnp.where(places < fixed, places, moved)]].set(jnp.asarray(sizes, jnp.int32))

    sizes = jnp.where(number % 4 == 0, named(crowded, number // 4), named(common, number - number // 4 - 1))
    mixed = jax.random.permutation(jax.random.fold_in(own, 3), number_of)
    giver, receiver = mixed[0:number_of // 2 * 2:2], mixed[1:number_of // 2 * 2:2]
    room = jnp.minimum(sizes[giver] - 1, most - sizes[receiver]) // 2
    room = jnp.where((giver == order[0]) | (receiver == order[0]) | (sizes[receiver] == 0), 0, jnp.maximum(room, 0))
    moved = jax.random.randint(jax.random.fold_in(own, 4), (number_of // 2,), 0, 1 << 20) % (room + 1)
    sizes = sizes.at[giver].add(-moved).at[receiver].add(moved)
    labels = jnp.searchsorted(jnp.cumsum(sizes), jnp.arange(rows * top), side="right").astype(jnp.int32)
    grid = labels.reshape(top, rows).T
    grid = grid[jax.random.permutation(jax.random.fold_in(own, 1), rows)]
    offset_by = jax.random.randint(jax.random.fold_in(own, 2), (rows, 1), 0, top)
    return jnp.take_along_axis(grid, (jnp.arange(top)[None, :] + offset_by) % top, axis=1)


def load_shares(amount, total, bound, lean, full):
    loads = [(1 << 20) // math.isqrt(standing ** lean) + 1 for standing in range(1, amount + 1)]
    largest = bound if full else min(bound, max(-(-total // amount), total * loads[0] // sum(loads)))
    least = 1 if total - largest >= amount - 1 else 0
    holding, spare = [largest] + [least] * (amount - 1), total - largest - least * (amount - 1)
    while spare > 0:
        free = [i for i in range(1, amount) if holding[i] < largest] or [i for i in range(1, amount) if holding[i] < bound]
        pool, left = sum([loads[i] for i in free]), spare
        for i in free:
            extra = min(bound - holding[i], max(1, left * loads[i] // pool), spare)
            holding[i] = holding[i] + extra
            spare = spare - extra
    return np.array(holding)


def noise(stream_key, dims, deviation, limit, pieces=(), kind=jnp.bfloat16):
    drawn = deviation * jax.random.normal(stream_key, dims, jnp.float32)
    if pieces:
        drawn = drawn * levels(stream_key, dims, pieces, -0.22, 0.18)
    return jnp.clip(drawn, -limit, limit).astype(kind)


def setup_inputs(seed: int = 0) -> dict:
    seeds = jax.random.split(jax.random.key(seed), 22)
    residual = draw_residual(jax.random.fold_in(seeds[21], 71), 0)
    in_gain = jnp.clip(1.0 + 0.18 * jax.random.normal(seeds[1], (D,), jnp.float32), 0.1, 1.9)
    in_weight = noise(seeds[2], (D, SW), D ** -0.5, 0.125, ((1, 4),))
    state = noise(seeds[3], (2, SEQS, GS), 0.5, 3.0, ((1, 8), (2, 4)), jnp.float32)
    decay_rate = jnp.clip(jnp.exp(math.log(1.0) - 2.3025851 * jax.random.uniform(seeds[4], (GROUPS, STATE), jnp.float32) ** levels(seeds[4], (GROUPS, STATE), ((0, 4),), -0.2, 0.2)), 0.1, 1.0)
    frequency = jnp.clip(200.0 * jax.random.uniform(seeds[5], (GROUPS, STATE), jnp.float32) ** levels(seeds[5], (GROUPS, STATE), ((0, 4),), -0.2, 0.2), 0.0, 200.0)
    log_step = jnp.clip(-3.0 + 2.3 * jax.random.uniform(seeds[6], (GROUPS,), jnp.float32) ** levels(seeds[6], (GROUPS,), ((0, 4),), -0.2, 0.2), -3.0, -0.7)
    in_coef = noise(seeds[7], (2, GROUPS, STATE, GROUP_CH), (2 * GROUP_CH) ** -0.5, 1.0, ((1, 4),), jnp.float32)
    out_coef = noise(seeds[8], (2, GROUPS, GROUP_CH, STATE), STATE ** -0.5, 0.75, ((1, 4),), jnp.float32)
    skip_gain = noise(seeds[9], (SW,), 0.5, 3.0, ((0, 4),), jnp.float32)
    out_weight = noise(seeds[10], (SW, D), SW ** -0.5, 0.1875)
    mid_gain = jnp.clip(1.0 + 0.18 * jax.random.normal(seeds[11], (D,), jnp.float32), 0.1, 1.9)
    gate_vector = noise(seeds[12], (D,), D ** -0.5, 0.125)
    routes_keys = jax.random.split(jax.random.fold_in(seeds[13], 1), SEQS // SEQ_DEV)
    routes_turns = jax.random.permutation(jax.random.fold_in(seeds[13], 3), SEQS // SEQ_DEV)
    routes = jax.vmap(lambda own, number: deal_out(jax.random.fold_in(seeds[13], 2), own, number, SEQ_DEV, EXPERTS, TOP, CAP, 2))(routes_keys, routes_turns).reshape((SEQS, TOP))
    route_weight = jnp.clip(jnp.exp(math.log(1.0) - 2.3025851 * jax.random.uniform(seeds[14], (SEQS, TOP), jnp.float32) ** levels(seeds[14], (SEQS, TOP), ((0, 8),), -0.2, 0.2)), 0.1, 1.0)
    expert_gate = noise(seeds[15], (EXPERTS, D, FF), D ** -0.5, 0.125, ((0, 32),))
    expert_up = noise(seeds[16], (EXPERTS, D, FF), D ** -0.5, 0.125, ((0, 32),))
    expert_down = noise(seeds[17], (EXPERTS, FF, D), FF ** -0.5, 0.25, ((0, 32),))
    shared_gate = noise(seeds[18], (D, SFF), D ** -0.5, 0.125, ((1, 8),))
    shared_up = noise(seeds[19], (D, SFF), D ** -0.5, 0.125, ((1, 8),))
    shared_down = noise(seeds[20], (SFF, D), SFF ** -0.5, 0.09375, ((0, 8),))
    return dict(residual=residual, in_gain=in_gain, in_weight=in_weight, state=state, decay_rate=decay_rate, frequency=frequency, log_step=log_step, in_coef=in_coef, out_coef=out_coef, skip_gain=skip_gain, out_weight=out_weight, mid_gain=mid_gain, gate_vector=gate_vector, routes=routes, route_weight=route_weight, expert_gate=expert_gate, expert_up=expert_up, expert_down=expert_down, shared_gate=shared_gate, shared_up=shared_up, shared_down=shared_down)


norm_eps = 1e-05
routed_scale = 2.5

def layer_norm(values, gain_vec):
    row_mean = lax.optimization_barrier(jnp.mean(values, axis=-1, keepdims=True))
    row_square = lax.optimization_barrier(jnp.mean(values * values, axis=-1, keepdims=True))
    return (values - row_mean) * lax.rsqrt(row_square - row_mean * row_mean + norm_eps) * gain_vec.astype(jnp.float32)

def coefficients(decay_rate, frequency, log_step, in_coef):
    time_step = jnp.exp(log_step)[:, None]
    real_rate = -decay_rate
    magnitude = jnp.exp(real_rate * time_step)
    keep_re = magnitude * jnp.cos(frequency * time_step)
    keep_im = magnitude * jnp.sin(frequency * time_step)
    denominator = real_rate * real_rate + frequency * frequency
    factor_re = ((keep_re - 1.0) * real_rate + keep_im * frequency) / denominator
    factor_im = (keep_im * real_rate - (keep_re - 1.0) * frequency) / denominator
    push_re = factor_re[..., None] * in_coef[0] - factor_im[..., None] * in_coef[1]
    push_im = factor_re[..., None] * in_coef[1] + factor_im[..., None] * in_coef[0]
    return (keep_re, keep_im, push_re, push_im)

def mixer_step(normed, in_weight, state, decay_rate, frequency, log_step, in_coef, out_coef, skip_gain):
    row_count = normed.shape[0]
    group_count, state_count = decay_rate.shape
    keep_re, keep_im, push_re, push_im = coefficients(decay_rate, frequency, log_step, in_coef)
    drive = jnp.dot(normed, in_weight, preferred_element_type=jnp.float32).astype(jnp.bfloat16)
    drive_f = drive.astype(jnp.float32).reshape(row_count, group_count, -1)
    highest = lax.Precision.HIGHEST
    input_re = jnp.einsum('tgh,gph->tgp', drive_f, push_re, precision=highest)
    input_im = jnp.einsum('tgh,gph->tgp', drive_f, push_im, precision=highest)
    old_re = state[0].reshape(row_count, group_count, state_count)
    old_im = state[1].reshape(row_count, group_count, state_count)
    new_re = keep_re * old_re - keep_im * old_im + input_re
    new_im = keep_re * old_im + keep_im * old_re + input_im
    read_out = jnp.einsum('ghp,tgp->tgh', out_coef[0], new_re, precision=highest) - jnp.einsum('ghp,tgp->tgh', out_coef[1], new_im, precision=highest)
    read_out = read_out.reshape(row_count, -1) + skip_gain * drive_f.reshape(row_count, -1)
    mixed_rows = jax.nn.gelu(read_out, approximate=True).astype(jnp.bfloat16)
    updated = jnp.stack([new_re.reshape(row_count, -1), new_im.reshape(row_count, -1)])
    return (mixed_rows, updated)

def route_slots(routes, experts):
    flat_routes = routes.reshape(-1)
    onehot = (flat_routes[:, None] == jnp.arange(experts, dtype=jnp.int32)[None, :]).astype(jnp.int32)
    before = jnp.cumsum(onehot, axis=0) - onehot
    return lax.optimization_barrier(jnp.sum(before * onehot, axis=1)).reshape(routes.shape)

def expert_block(row_block, gate_weight, up_weight, down_weight):
    gate_part = jnp.dot(row_block, gate_weight, preferred_element_type=jnp.float32)
    up_part = jnp.dot(row_block, up_weight, preferred_element_type=jnp.float32)
    hidden = (jax.nn.silu(gate_part) * up_part).astype(jnp.bfloat16)
    return jnp.dot(hidden, down_weight, preferred_element_type=jnp.float32).astype(jnp.bfloat16)

def reference(residual, in_gain, in_weight, state, decay_rate, frequency, log_step, in_coef, out_coef, skip_gain, out_weight, mid_gain, gate_vector, routes, route_weight, expert_gate, expert_up, expert_down, shared_gate, shared_up, shared_down):
    resid_f = residual.astype(jnp.float32)
    normed = layer_norm(resid_f, in_gain).astype(jnp.bfloat16)
    mixed_rows, new_state = mixer_step(normed, in_weight, state, decay_rate, frequency, log_step, in_coef, out_coef, skip_gain)
    after_mix = resid_f + jnp.dot(mixed_rows, out_weight, preferred_element_type=jnp.float32)
    normed_mid = layer_norm(after_mix, mid_gain).astype(jnp.bfloat16)
    slot_rank = jax.vmap(route_slots, in_axes=(0, None))(routes.reshape(N_EP, SEQ_DEV, TOP), EXPERTS).reshape(SEQS, TOP)
    group_of = (jnp.arange(SEQS, dtype=jnp.int32) // SEQ_DEV)[:, None]
    slot_place = routes * (N_EP * CAP) + group_of * CAP + slot_rank
    token_ids = jnp.broadcast_to(jnp.arange(SEQS, dtype=jnp.int32)[:, None], slot_place.shape)
    slot_token = jnp.zeros((EXPERTS * N_EP * CAP,), jnp.int32).at[slot_place.reshape(-1)].set(token_ids.reshape(-1))
    buffer = normed_mid[slot_token].reshape(EXPERTS, N_EP * CAP, D)
    outputs = lax.map(lambda packed: expert_block(*packed), (buffer, expert_gate, expert_up, expert_down)).reshape(EXPERTS * N_EP * CAP, D)
    weights = route_weight / lax.optimization_barrier(jnp.sum(route_weight, axis=-1, keepdims=True)) * routed_scale
    routed = lax.optimization_barrier(jnp.sum(weights[..., None] * outputs[slot_place].astype(jnp.float32), axis=1))
    gate_part = jnp.dot(normed_mid, shared_gate, preferred_element_type=jnp.float32)
    up_part = jnp.dot(normed_mid, shared_up, preferred_element_type=jnp.float32)
    shared_hidden = (jax.nn.silu(gate_part) * up_part).astype(jnp.bfloat16)
    shared = jnp.dot(shared_hidden, shared_down, preferred_element_type=jnp.float32)
    gate_value = jax.nn.sigmoid(jnp.dot(normed_mid, gate_vector, preferred_element_type=jnp.float32))
    layer_out = (after_mix + routed + gate_value[:, None] * shared).astype(jnp.bfloat16)
    return (layer_out, new_state)
```

```python
import functools
import itertools

import jax
import jax.numpy as jnp
from jax import lax
from jax.experimental import pallas as pl
from jax.experimental.pallas import tpu as pltpu
from jax.sharding import PartitionSpec as P

norm_eps = 1e-05
routed_scale = 2.5
lanes = 128


def layer_norm(values, gain_vec):
    row_mean = jnp.mean(values, axis=-1, keepdims=True)
    row_square = jnp.mean(values * values, axis=-1, keepdims=True)
    return (values - row_mean) * lax.rsqrt(row_square - row_mean * row_mean + norm_eps) * gain_vec


def coefficients(decay_rate, frequency, log_step, in_coef):
    time_step = jnp.exp(log_step)[:, None]
    real_rate = -decay_rate
    magnitude = jnp.exp(real_rate * time_step)
    keep_re = magnitude * jnp.cos(frequency * time_step)
    keep_im = magnitude * jnp.sin(frequency * time_step)
    denominator = real_rate * real_rate + frequency * frequency
    factor_re = ((keep_re - 1.0) * real_rate + keep_im * frequency) / denominator
    factor_im = (keep_im * real_rate - (keep_re - 1.0) * frequency) / denominator
    push_re = factor_re[..., None] * in_coef[0] - factor_im[..., None] * in_coef[1]
    push_im = factor_re[..., None] * in_coef[1] + factor_im[..., None] * in_coef[0]
    return (keep_re, keep_im, push_re, push_im)


def mixer_step(
    normed, in_weight, state, decay_rate, frequency, log_step, in_coef, out_coef, skip_gain
):
    row_count = normed.shape[0]
    group_count, state_count = decay_rate.shape
    keep_re, keep_im, push_re, push_im = coefficients(decay_rate, frequency, log_step, in_coef)
    drive = jnp.dot(normed, in_weight, preferred_element_type=jnp.float32).astype(jnp.bfloat16)
    drive_f = drive.astype(jnp.float32).reshape(row_count, group_count, -1)
    highest = lax.Precision.HIGHEST
    input_re = jnp.einsum("tgh,gph->tgp", drive_f, push_re, precision=highest)
    input_im = jnp.einsum("tgh,gph->tgp", drive_f, push_im, precision=highest)
    old_re = state[0].reshape(row_count, group_count, state_count)
    old_im = state[1].reshape(row_count, group_count, state_count)
    new_re = keep_re * old_re - keep_im * old_im + input_re
    new_im = keep_re * old_im + keep_im * old_re + input_im
    read_out = jnp.einsum("ghp,tgp->tgh", out_coef[0], new_re, precision=highest) - jnp.einsum(
        "ghp,tgp->tgh", out_coef[1], new_im, precision=highest
    )
    read_out = read_out.reshape(row_count, -1) + skip_gain * drive_f.reshape(row_count, -1)
    mixed_rows = jax.nn.gelu(read_out, approximate=True).astype(jnp.bfloat16)
    updated = jnp.stack([new_re.reshape(row_count, -1), new_im.reshape(row_count, -1)])
    return (mixed_rows, updated)


def grid_sizes(ep_count, tp_count):
    inner = max(k for k in range(1, ep_count + 1) if ep_count % k == 0 and k * k <= ep_count)
    return {"z": ep_count // inner, "x": inner, "y": tp_count // 2, "c": 2}


def place_of(sizes):
    ep_place, tp_place = lax.axis_index("ep"), lax.axis_index("tp")
    return {
        "z": ep_place // sizes["x"],
        "x": ep_place % sizes["x"],
        "y": tp_place // 2,
        "c": tp_place % 2,
    }


def moved(sizes, place, offset):
    return {
        axis: (place[axis] + offset[axis]) % sizes[axis] if offset.get(axis) else place[axis]
        for axis in place
    }


def device_at(sizes, place):
    return {"ep": place["z"] * sizes["x"] + place["x"], "tp": place["y"] * 2 + place["c"]}


def block_at(sizes, axes, place):
    index = 0
    for axis in axes:
        index = index * sizes[axis] + place[axis]
    return index


def rank_at(sizes, axes, offset):
    return block_at(sizes, axes, {axis: offset.get(axis, 0) for axis in axes})


def greet(sizes, axes, place):
    barrier = pltpu.get_barrier_semaphore()
    count = 0
    for axis in axes:
        for step in range(1, sizes[axis]):
            pl.semaphore_signal(
                barrier,
                inc=1,
                device_id=device_at(sizes, moved(sizes, place, {axis: step})),
                device_id_type=pl.DeviceIdType.MESH,
            )
            count += 1
    pl.semaphore_wait(barrier, count)


def offsets_over(sizes, axes):
    for steps in itertools.product(*[range(sizes[axis]) for axis in axes]):
        yield dict(zip(axes, steps))


def gather_kernel(sizes, axes, parts, in_ref, out_ref, send_sem, recv_sem, own_sem):
    place = place_of(sizes)
    total = 1
    for axis in axes:
        total *= sizes[axis]
    own = block_at(sizes, axes, place)
    own_copy = pltpu.make_async_copy(in_ref, out_ref.at[own], own_sem)
    own_copy.start()
    greet(sizes, axes, place)

    def columns(ref, part):
        return ref.at[:, pl.ds(parts[part][1], parts[part][2])]

    def copy_of(source, part, block, rank, peer):
        return pltpu.make_async_remote_copy(
            src_ref=columns(source, part),
            dst_ref=columns(out_ref.at[block], part),
            send_sem=send_sem,
            recv_sem=recv_sem.at[part, rank],
            device_id=device_at(sizes, peer),
            device_id_type=pl.DeviceIdType.MESH,
        )

    for stage in range(len(axes) + 1):
        lists = []
        for part, (order, _, _) in enumerate(parts):
            todo = []
            if stage == 0:
                todo.append({})
            else:
                for offset in offsets_over(sizes, order[:stage]):
                    if offset[order[stage - 1]]:
                        todo.append(offset)
                todo.sort(key=lambda o: [bool(o[a]) for a in order[:stage]])
            lists.append([(part, order, offset) for offset in todo])
        for items in itertools.zip_longest(*lists):
            for item in items:
                if item is None:
                    continue
                part, order, offset = item
                block = block_at(sizes, axes, moved(sizes, place, offset))
                source = in_ref if stage == 0 else out_ref.at[block]
                if stage:
                    copy_of(
                        source, part, block, rank_at(sizes, axes, offset), moved(sizes, place, {order[0]: 1})
                    ).wait_recv()
                for axis in order[stage:]:
                    for step in range(1, sizes[axis]):
                        seen = dict(offset)
                        seen[axis] = sizes[axis] - step
                        copy_of(
                            source,
                            part,
                            block,
                            rank_at(sizes, axes, seen),
                            moved(sizes, place, {axis: step}),
                        ).start()
    own_copy.wait()
    sent = out_ref.at[pl.ds(0, total - 1)]
    pltpu.make_async_copy(sent, sent, send_sem).wait()


def gather_blocks(sizes, axes, parts, block, collective_id):
    total = 1
    for axis in axes:
        total *= sizes[axis]
    vmem = pl.BlockSpec(memory_space=pltpu.VMEM)
    return pl.pallas_call(
        functools.partial(gather_kernel, sizes, axes, parts),
        out_shape=jax.ShapeDtypeStruct((total,) + block.shape, block.dtype),
        in_specs=[vmem],
        out_specs=vmem,
        scratch_shapes=[
            pltpu.SemaphoreType.DMA,
            pltpu.SemaphoreType.DMA((len(parts), total)),
            pltpu.SemaphoreType.DMA,
        ],
        compiler_params=pltpu.CompilerParams(collective_id=collective_id, has_side_effects=True),
    )(block)


def scatter_kernel(
    sizes, axes, parts, in_ref, base_ref, out_ref, recv_ref, sum_ref, send_sem, recv_sem
):
    place = place_of(sizes)
    total = in_ref.shape[0]
    half = parts[0][2]
    greet(sizes, axes, place)
    slot_at = [0] * len(parts)
    waiting = []

    def flush():
        for copy in waiting:
            copy.start()
        waiting.clear()

    def columns(ref, part):
        return ref.at[:, pl.ds(parts[part][1], half)]

    def held(part, order, stage, offset):
        if stage == 0:
            return columns(in_ref.at[block_at(sizes, axes, moved(sizes, place, offset))], part)
        return sum_ref.at[part, rank_at(sizes, order[1:], offset)]

    def slot_of(part, order, stage, step, offset):
        rest = order[stage + 1 :]
        count = 1
        for axis in rest:
            count *= sizes[axis]
        return slot_at[part] + (step - 1) * count + rank_at(sizes, rest, offset)

    def send_of(part, order, stage, offset):
        axis = order[stage]
        slot = slot_of(part, order, stage, offset[axis], offset)
        return pltpu.make_async_remote_copy(
            src_ref=held(part, order, stage, offset),
            dst_ref=recv_ref.at[part, slot],
            send_sem=send_sem,
            recv_sem=recv_sem.at[part, slot],
            device_id=device_at(sizes, moved(sizes, place, {axis: offset[axis]})),
            device_id_type=pl.DeviceIdType.MESH,
        )

    def sorted_offsets(order, stage):
        todo = list(offsets_over(sizes, order[stage:]))
        todo.sort(key=lambda o: [not o[axis] for axis in order[stage:]])
        return todo

    def interleave(lists):
        for items in itertools.zip_longest(*lists):
            for item in items:
                if item is not None:
                    yield item

    firsts = []
    for part, (order, _, _) in enumerate(parts):
        todo = [o for o in sorted_offsets(order, 0) if o[order[0]]]
        firsts.append([(part, order, o) for o in todo])
    for part, order, offset in interleave(firsts):
        send_of(part, order, 0, offset).start()
    depth = len(axes)
    for stage in range(depth):
        lists = []
        for part, (order, _, _) in enumerate(parts):
            lists.append([(part, order, o) for o in sorted_offsets(order, stage + 1)])
        begun = list(slot_at)
        for part, order, offset in interleave(lists):
            before = dict(offset)
            before[order[stage]] = 0
            value = held(part, order, stage, before)[...].astype(jnp.float32)
            for step in range(1, sizes[order[stage]]):
                slot = slot_of(part, order, stage, step, offset)
                arrived = recv_ref.at[part, slot]
                pltpu.make_async_copy(arrived, arrived, recv_sem.at[part, slot]).wait()
                value = value + arrived[...].astype(jnp.float32)
            if stage == depth - 1:
                where = pl.ds(parts[part][1], half)
                out_ref[:, where] = (base_ref[:, where] + value).astype(out_ref.dtype)
                continue
            sum_ref[part, rank_at(sizes, order[1:], offset)] = value.astype(sum_ref.dtype)
            flush()
            if offset[order[stage + 1]]:
                count = 1
                for axis in order[stage + 1 :]:
                    count *= sizes[axis]
                slot_at[part] = begun[part] + (sizes[order[stage]] - 1) * count
                waiting.append(send_of(part, order, stage + 1, offset))
                slot_at[part] = begun[part]
        flush()
        for part, (order, _, _) in enumerate(parts):
            count = 1
            for axis in order[stage + 1 :]:
                count *= sizes[axis]
            slot_at[part] = begun[part] + (sizes[order[stage]] - 1) * count
    for part in range(len(parts)):
        sent = recv_ref.at[part]
        pltpu.make_async_copy(sent, sent, send_sem).wait()


def scatter_blocks(sizes, axes, parts, blocks, base, collective_id):
    total, rows, width = blocks.shape
    half = parts[0][2]
    vmem = pl.BlockSpec(memory_space=pltpu.VMEM)
    return pl.pallas_call(
        functools.partial(scatter_kernel, sizes, axes, parts),
        out_shape=jax.ShapeDtypeStruct((rows, width), jnp.bfloat16),
        in_specs=[vmem, vmem],
        out_specs=vmem,
        scratch_shapes=[
            pltpu.VMEM((len(parts), total - 1, rows, half), jnp.bfloat16),
            pltpu.VMEM((len(parts), total // 2, rows, half), jnp.bfloat16),
            pltpu.SemaphoreType.DMA,
            pltpu.SemaphoreType.DMA((len(parts), total)),
        ],
        compiler_params=pltpu.CompilerParams(
            collective_id=collective_id, has_side_effects=True, vmem_limit_bytes=48 * 2**20
        ),
    )(blocks, base)


def three_terms(values):
    first = values.astype(jnp.bfloat16)
    rest = values - first.astype(jnp.float32)
    second = rest.astype(jnp.bfloat16)
    third = (rest - second.astype(jnp.float32)).astype(jnp.bfloat16)
    return [first, second, third]


def per_device(
    residual,
    in_gain,
    in_weight,
    state,
    decay_rate,
    frequency,
    log_step,
    in_coef,
    out_coef,
    skip_gain,
    out_weight,
    mid_gain,
    gate_vector,
    routes,
    route_weight,
    expert_gate,
    expert_up,
    expert_down,
    shared_gate,
    shared_up,
    shared_down,
):
    tp_count = lax.axis_size("tp")
    ep_count = lax.axis_size("ep")
    tp_place = lax.axis_index("tp")
    ep_place = lax.axis_index("ep")
    seq_rows, feat_part = residual.shape
    width = feat_part * tp_count
    per_dev = seq_rows // tp_count
    experts = ep_count * tp_count
    top_count = routes.shape[1]
    capacity = max(2, 2 * seq_rows * top_count // experts)
    sizes = grid_sizes(ep_count, tp_count)

    def gather_features(values, collective_id):
        parts = [("yc", 0, values.shape[1])]
        blocks = gather_blocks(sizes, "yc", parts, values, collective_id)
        return jnp.swapaxes(blocks, 0, 1).reshape(seq_rows, -1)

    full_resid = gather_features(residual, 0).astype(jnp.float32)
    normed = layer_norm(full_resid, in_gain).astype(jnp.bfloat16)
    mixed_part, new_state = mixer_step(
        normed, in_weight, state, decay_rate, frequency, log_step, in_coef, out_coef, skip_gain
    )
    mixed_rows = gather_features(mixed_part, 1)

    own_rows = lambda values: lax.dynamic_slice_in_dim(values, tp_place * per_dev, per_dev, 0)
    own_after = own_rows(full_resid) + jnp.dot(
        own_rows(mixed_rows), out_weight, preferred_element_type=jnp.float32
    )
    own_mid = layer_norm(own_after, mid_gain).astype(jnp.bfloat16)
    weights = route_weight / jnp.sum(route_weight, axis=-1, keepdims=True) * routed_scale
    tail = [own_rows(routes).astype(jnp.bfloat16)] + three_terms(own_rows(weights))
    tail.append(jnp.zeros((per_dev, lanes - 4 * top_count), jnp.bfloat16))
    sent = jnp.concatenate([own_mid] + tail, axis=1)
    half = width // 2
    parts = [("zxyc", 0, half), ("zyxc", half, sent.shape[1] - half)]
    got = gather_blocks(sizes, "zxyc", parts, sent, 2).reshape(-1, sent.shape[1])

    rows = got[:, :width].reshape(ep_count, seq_rows, width)
    extra = got[:, width:].astype(jnp.float32)
    ids = extra[:, :top_count]
    parts = [extra[:, top_count * k : top_count * (k + 1)] for k in (1, 2, 3)]
    weight_of = (parts[0] + parts[1]) + parts[2]
    mine = (ep_place * tp_count + tp_place).astype(jnp.float32)
    hits = ids == mine
    hit = jnp.any(hits, axis=1).reshape(ep_count, seq_rows)
    hit_weight = jnp.sum(jnp.where(hits, weight_of, 0.0), axis=1).reshape(ep_count, seq_rows)
    places = jnp.arange(seq_rows)
    earlier = (places[:, None] < places[None, :]).astype(jnp.bfloat16)
    rank = jnp.dot(hit.astype(jnp.bfloat16), earlier, preferred_element_type=jnp.float32)
    chosen = hit[:, None, :] & (
        rank[:, None, :] == jnp.arange(capacity, dtype=jnp.float32)[None, :, None]
    )
    onehot = chosen.astype(jnp.bfloat16)
    slot_weight = jnp.sum(jnp.where(chosen, hit_weight[:, None, :], 0.0), axis=2)
    picked = jnp.einsum("gjr,grd->gjd", onehot, rows, preferred_element_type=jnp.float32)
    picked = picked.astype(jnp.bfloat16).reshape(ep_count * capacity, width)

    def two_layers(values, gate_weight, up_weight, down_weight):
        gate_part = jnp.dot(values, gate_weight, preferred_element_type=jnp.float32)
        up_part = jnp.dot(values, up_weight, preferred_element_type=jnp.float32)
        hidden = (jax.nn.silu(gate_part) * up_part).astype(jnp.bfloat16)
        return jnp.dot(hidden, down_weight, preferred_element_type=jnp.float32)

    result = two_layers(picked, expert_gate[0], expert_up[0], expert_down[0])
    result = (result * slot_weight.reshape(-1)[:, None]).astype(jnp.bfloat16)
    spread = jnp.einsum(
        "gjr,gjd->grd",
        onehot,
        result.reshape(ep_count, capacity, width),
        preferred_element_type=jnp.float32,
    )
    piece = lax.dynamic_slice_in_dim(rows, tp_place * per_dev, per_dev, 1).reshape(-1, width)
    gate_value = jax.nn.sigmoid(jnp.dot(piece, gate_vector, preferred_element_type=jnp.float32))
    shared = two_layers(piece, shared_gate, shared_up, shared_down) * gate_value[:, None]
    is_own = (jnp.arange(tp_count) == tp_place)[None, :, None, None]
    total = spread.reshape(ep_count, tp_count, per_dev, width) + jnp.where(
        is_own, shared.reshape(ep_count, 1, per_dev, width), 0.0
    )
    total = total.astype(jnp.bfloat16).reshape(-1, per_dev, width)
    parts = [("cyxz", 0, half), ("cxyz", half, half)]
    layer_out = scatter_blocks(sizes, "zxyc", parts, total, own_after, 3)
    return (layer_out, new_state)


def solution(mesh):
    return jax.shard_map(
        per_device,
        mesh=mesh,
        in_specs=(
            P("ep", "tp"),
            P(),
            P(None, "tp"),
            P(None, "ep", "tp"),
            P("tp", None),
            P("tp", None),
            P("tp"),
            P(None, "tp", None, None),
            P(None, "tp", None, None),
            P("tp"),
            P(),
            P(),
            P(),
            P("ep", None),
            P("ep", None),
            P(("ep", "tp"), None, None),
            P(("ep", "tp"), None, None),
            P(("ep", "tp"), None, None),
            P(None, "ep"),
            P(None, "ep"),
            P("ep", None),
        ),
        out_specs=(P(("ep", "tp"), None), P(None, "ep", "tp")),
        check_vma=False,
    )
```

```python
import functools
import itertools

import jax
import jax.numpy as jnp
from jax import lax
from jax.experimental import pallas as pl
from jax.experimental.pallas import tpu as pltpu
from jax.sharding import PartitionSpec as P

norm_eps = 1e-05
routed_scale = 2.5
lanes = 128


def layer_norm(values, gain_vec):
    row_mean = jnp.mean(values, axis=-1, keepdims=True)
    row_square = jnp.mean(values * values, axis=-1, keepdims=True)
    return (values - row_mean) * lax.rsqrt(row_square - row_mean * row_mean + norm_eps) * gain_vec


def coefficients(decay_rate, frequency, log_step, in_coef):
    time_step = jnp.exp(log_step)[:, None]
    real_rate = -decay_rate
    magnitude = jnp.exp(real_rate * time_step)
    keep_re = magnitude * jnp.cos(frequency * time_step)
    keep_im = magnitude * jnp.sin(frequency * time_step)
    denominator = real_rate * real_rate + frequency * frequency
    factor_re = ((keep_re - 1.0) * real_rate + keep_im * frequency) / denominator
    factor_im = (keep_im * real_rate - (keep_re - 1.0) * frequency) / denominator
    push_re = factor_re[..., None] * in_coef[0] - factor_im[..., None] * in_coef[1]
    push_im = factor_re[..., None] * in_coef[1] + factor_im[..., None] * in_coef[0]
    return (keep_re, keep_im, push_re, push_im)


def mixer_kernel(
    normed_ref,
    in_weight_ref,
    state_ref,
    keep_ref,
    push_ref,
    pull_ref,
    skip_ref,
    mixed_ref,
    new_ref,
):
    highest = lax.Precision.HIGHEST
    drive = jnp.dot(normed_ref[...], in_weight_ref[...], preferred_element_type=jnp.float32)
    drive = drive.astype(jnp.bfloat16).astype(jnp.float32)

    def product(left, right):
        return jnp.dot(left, right, precision=highest, preferred_element_type=jnp.float32)

    shape = (drive.shape[1], state_ref.shape[2])
    group_ch = push_ref.shape[1]
    copies = shape[0] // group_ch
    row_group = lax.broadcasted_iota(jnp.int32, shape, 0) // group_ch
    entry_group = lax.broadcasted_iota(jnp.int32, shape, 1) // (shape[1] // copies)
    same = row_group == entry_group

    def dense(values):
        return jnp.where(same, jnp.concatenate([values] * copies, axis=0), 0.0)

    def product_t(left, right):
        return lax.dot_general(
            left,
            right,
            (((1,), (1,)), ((), ())),
            precision=highest,
            preferred_element_type=jnp.float32,
        )

    keep_re, keep_im = keep_ref[0:1, :], keep_ref[1:2, :]
    old_re, old_im = state_ref[0], state_ref[1]
    new_re = keep_re * old_re - keep_im * old_im + product(drive, dense(push_ref[0]))
    new_im = keep_re * old_im + keep_im * old_re + product(drive, dense(push_ref[1]))
    new_ref[0] = new_re
    new_ref[1] = new_im
    read_out = product_t(new_re, dense(pull_ref[0])) - product_t(new_im, dense(pull_ref[1]))
    read_out = read_out + skip_ref[...] * drive
    mixed_ref[...] = jax.nn.gelu(read_out, approximate=True).astype(mixed_ref.dtype)


def mixer_step(
    normed, in_weight, state, decay_rate, frequency, log_step, in_coef, out_coef, skip_gain
):
    rows = normed.shape[0]
    groups, entries = decay_rate.shape
    channels = in_weight.shape[1]
    keep_re, keep_im, push_re, push_im = coefficients(decay_rate, frequency, log_step, in_coef)
    keep = jnp.stack([keep_re.reshape(-1), keep_im.reshape(-1)])
    push = jnp.stack([push_re, push_im]).transpose(0, 3, 1, 2).reshape(2, -1, groups * entries)
    pull = out_coef.transpose(0, 2, 1, 3).reshape(2, -1, groups * entries)
    vmem = pl.BlockSpec(memory_space=pltpu.VMEM)
    return pl.pallas_call(
        mixer_kernel,
        out_shape=(
            jax.ShapeDtypeStruct((rows, channels), jnp.bfloat16),
            jax.ShapeDtypeStruct(state.shape, jnp.float32),
        ),
        in_specs=[vmem] * 7,
        out_specs=(vmem, vmem),
        compiler_params=pltpu.CompilerParams(vmem_limit_bytes=24 * 2**20),
    )(normed, in_weight, state, keep, push, pull, skip_gain.reshape(1, -1))


def grid_sizes(ep_count, tp_count):
    inner = max(k for k in range(1, ep_count + 1) if ep_count % k == 0 and k * k <= ep_count)
    return {"z": ep_count // inner, "x": inner, "y": tp_count // 2, "c": 2}


def place_of(sizes):
    ep_place, tp_place = lax.axis_index("ep"), lax.axis_index("tp")
    return {
        "z": ep_place // sizes["x"],
        "x": ep_place % sizes["x"],
        "y": tp_place // 2,
        "c": tp_place % 2,
    }


def moved(sizes, place, offset):
    return {
        axis: (place[axis] + offset[axis]) % sizes[axis] if offset.get(axis) else place[axis]
        for axis in place
    }


def device_at(sizes, place):
    return {"ep": place["z"] * sizes["x"] + place["x"], "tp": place["y"] * 2 + place["c"]}


def block_at(sizes, axes, place):
    index = 0
    for axis in axes:
        index = index * sizes[axis] + place[axis]
    return index


def rank_at(sizes, axes, offset):
    return block_at(sizes, axes, {axis: offset.get(axis, 0) for axis in axes})


def greet(sizes, axes, place):
    barrier = pltpu.get_barrier_semaphore()
    count = 0
    for axis in axes:
        for step in range(1, sizes[axis]):
            pl.semaphore_signal(
                barrier,
                inc=1,
                device_id=device_at(sizes, moved(sizes, place, {axis: step})),
                device_id_type=pl.DeviceIdType.MESH,
            )
            count += 1
    pl.semaphore_wait(barrier, count)


def offsets_over(sizes, axes):
    for steps in itertools.product(*[range(sizes[axis]) for axis in axes]):
        yield dict(zip(axes, steps))


def gather_kernel(sizes, axes, parts, wide, in_ref, out_ref, send_sem, recv_sem, own_sem):
    place = place_of(sizes)
    total = 1
    for axis in axes:
        total *= sizes[axis]
    own = block_at(sizes, axes, place)

    def spot(block):
        if wide:
            cols = in_ref.shape[1]
            return out_ref.at[:, pl.ds(pl.multiple_of(block * cols, lanes), cols)]
        return out_ref.at[block]

    own_copy = pltpu.make_async_copy(in_ref, spot(own), own_sem)
    own_copy.start()
    greet(sizes, axes, place)

    def columns(ref, part):
        return ref if wide else ref.at[:, pl.ds(parts[part][1], parts[part][2])]

    def copy_of(source, part, block, rank, peer):
        return pltpu.make_async_remote_copy(
            src_ref=columns(source, part),
            dst_ref=columns(spot(block), part),
            send_sem=send_sem,
            recv_sem=recv_sem.at[part, rank],
            device_id=device_at(sizes, peer),
            device_id_type=pl.DeviceIdType.MESH,
        )

    events = []
    for part, (order, _, _) in enumerate(parts):
        delays = {axis: 2.5 + k for k, axis in enumerate(order)}
        for offset in offsets_over(sizes, order):
            steps = {axis: (sizes[axis] - offset[axis]) % sizes[axis] for axis in order}
            arrival = sum(delays[axis] * steps[axis] for axis in order)
            events.append((arrival, part, offset))
    events.sort(key=lambda event: event[:2])
    for _, part, offset in events:
        order = parts[part][0]
        stage = max([k + 1 for k, axis in enumerate(order) if offset[axis]], default=0)
        block = block_at(sizes, axes, moved(sizes, place, offset))
        source = spot(block) if stage else in_ref
        if stage:
            rank = rank_at(sizes, axes, offset)
            copy_of(source, part, block, rank, moved(sizes, place, {order[0]: 1})).wait_recv()
        for axis in order[stage:]:
            for step in range(1, sizes[axis]):
                seen = dict(offset)
                seen[axis] = sizes[axis] - step
                peer = moved(sizes, place, {axis: step})
                copy_of(source, part, block, rank_at(sizes, axes, seen), peer).start()
    own_copy.wait()
    most = total - 1
    sent = out_ref.at[:, pl.ds(0, most * in_ref.shape[1])] if wide else out_ref.at[pl.ds(0, most)]
    pltpu.make_async_copy(sent, sent, send_sem).wait()


def gather_blocks(sizes, axes, parts, block, collective_id, wide=False):
    total = 1
    for axis in axes:
        total *= sizes[axis]
    rows, cols = block.shape
    shape = (rows, total * cols) if wide else (total, rows, cols)
    vmem = pl.BlockSpec(memory_space=pltpu.VMEM)
    return pl.pallas_call(
        functools.partial(gather_kernel, sizes, axes, parts, wide),
        out_shape=jax.ShapeDtypeStruct(shape, block.dtype),
        in_specs=[vmem],
        out_specs=vmem,
        scratch_shapes=[
            pltpu.SemaphoreType.DMA,
            pltpu.SemaphoreType.DMA((len(parts), total)),
            pltpu.SemaphoreType.DMA,
        ],
        compiler_params=pltpu.CompilerParams(
            collective_id=collective_id,
            has_side_effects=True,
            vmem_limit_bytes=(total + 2) * rows * cols * 2 + 4 * 2**20,
        ),
    )(block)


def scatter_kernel(
    sizes, axes, parts, in_ref, base_ref, out_ref, recv_ref, sum_ref, send_sem, recv_sem
):
    place = place_of(sizes)
    total = in_ref.shape[0]
    half = parts[0][2]
    greet(sizes, axes, place)
    waiting = []

    def flush():
        for copy in waiting:
            copy.start()
        waiting.clear()

    def columns(ref, part):
        return ref.at[:, pl.ds(parts[part][1], half)]

    def held(part, order, stage, offset):
        if stage == 0:
            return columns(in_ref.at[block_at(sizes, axes, moved(sizes, place, offset))], part)
        return sum_ref.at[part, rank_at(sizes, order[1:], offset)]

    def slot_of(part, order, stage, step, offset):
        base, left = 0, total
        for axis in order[:stage]:
            left //= sizes[axis]
            base += (sizes[axis] - 1) * left
        rest = order[stage + 1 :]
        count = left // sizes[order[stage]]
        return base + (step - 1) * count + rank_at(sizes, rest, offset)

    def send_of(part, order, stage, offset):
        axis = order[stage]
        slot = slot_of(part, order, stage, offset[axis], offset)
        return pltpu.make_async_remote_copy(
            src_ref=held(part, order, stage, offset),
            dst_ref=recv_ref.at[part, slot],
            send_sem=send_sem,
            recv_sem=recv_sem.at[part, slot],
            device_id=device_at(sizes, moved(sizes, place, {axis: offset[axis]})),
            device_id_type=pl.DeviceIdType.MESH,
        )

    far = sizes["z"] // 2

    def urgency(offset):
        return abs(offset["z"] - far) if offset["z"] else sizes["z"]

    firsts = []
    depth = len(axes)
    events = []
    for part, (order, _, _) in enumerate(parts):
        for offset in offsets_over(sizes, order):
            if offset[order[0]]:
                key = (urgency(offset), [not offset[axis] for axis in order])
                firsts.append((key, part, offset))
        for stage in range(depth):
            for offset in offsets_over(sizes, order[stage + 1 :]):
                z_step = offset.get("z", 0)
                when = 3.0 * urgency({"z": z_step}) + 3.0 * stage
                key = (when, [not offset[axis] for axis in order[stage + 1 :]])
                if stage == depth - 1:
                    key = (1e9, [])
                events.append((key, part, stage, offset))
    firsts.sort(key=lambda item: item[:2])
    events.sort(key=lambda item: item[:3])
    for _, part, offset in firsts:
        send_of(part, parts[part][0], 0, offset).start()
    for _, part, stage, offset in events:
        order = parts[part][0]
        before = dict(offset)
        before[order[stage]] = 0
        value = held(part, order, stage, before)[...].astype(jnp.float32)
        for step in range(1, sizes[order[stage]]):
            slot = slot_of(part, order, stage, step, offset)
            arrived = recv_ref.at[part, slot]
            if stage == depth - 1:
                flush()
            pltpu.make_async_copy(arrived, arrived, recv_sem.at[part, slot]).wait()
            value = value + arrived[...].astype(jnp.float32)
        if stage == depth - 1:
            where = pl.ds(parts[part][1], half)
            out_ref[:, where] = (base_ref[:, where] + value).astype(out_ref.dtype)
            continue
        sum_ref[part, rank_at(sizes, order[1:], offset)] = value.astype(sum_ref.dtype)
        flush()
        if offset[order[stage + 1]]:
            waiting.append(send_of(part, order, stage + 1, offset))
    for part in range(len(parts)):
        sent = recv_ref.at[part]
        pltpu.make_async_copy(sent, sent, send_sem).wait()


def scatter_blocks(sizes, axes, parts, blocks, base, collective_id):
    total, rows, width = blocks.shape
    half = parts[0][2]
    vmem = pl.BlockSpec(memory_space=pltpu.VMEM)
    return pl.pallas_call(
        functools.partial(scatter_kernel, sizes, axes, parts),
        out_shape=jax.ShapeDtypeStruct((rows, width), jnp.bfloat16),
        in_specs=[vmem, vmem],
        out_specs=vmem,
        scratch_shapes=[
            pltpu.VMEM((len(parts), total - 1, rows, half), jnp.bfloat16),
            pltpu.VMEM((len(parts), total // 2, rows, half), jnp.bfloat16),
            pltpu.SemaphoreType.DMA,
            pltpu.SemaphoreType.DMA((len(parts), total)),
        ],
        compiler_params=pltpu.CompilerParams(
            collective_id=collective_id, has_side_effects=True, vmem_limit_bytes=(3 * total) * rows * width * 2 + 4 * 2**20
        ),
    )(blocks, base)


def three_terms(values):
    first = values.astype(jnp.bfloat16)
    rest = values - first.astype(jnp.float32)
    second = rest.astype(jnp.bfloat16)
    third = (rest - second.astype(jnp.float32)).astype(jnp.bfloat16)
    return [first, second, third]


def per_device(
    residual,
    in_gain,
    in_weight,
    state,
    decay_rate,
    frequency,
    log_step,
    in_coef,
    out_coef,
    skip_gain,
    out_weight,
    mid_gain,
    gate_vector,
    routes,
    route_weight,
    expert_gate,
    expert_up,
    expert_down,
    shared_gate,
    shared_up,
    shared_down,
):
    tp_count = lax.axis_size("tp")
    ep_count = lax.axis_size("ep")
    tp_place = lax.axis_index("tp")
    ep_place = lax.axis_index("ep")
    seq_rows, feat_part = residual.shape
    width = feat_part * tp_count
    per_dev = seq_rows // tp_count
    experts = ep_count * tp_count
    top_count = routes.shape[1]
    capacity = max(2, 2 * seq_rows * top_count // experts)
    sizes = grid_sizes(ep_count, tp_count)

    def gather_features(values, collective_id):
        parts = [("yc", 0, values.shape[1])]
        return gather_blocks(sizes, "yc", parts, values, collective_id, wide=True)

    full_resid = gather_features(residual, 0).astype(jnp.float32)
    normed = layer_norm(full_resid, in_gain).astype(jnp.bfloat16)
    mixed_part, new_state = mixer_step(
        normed, in_weight, state, decay_rate, frequency, log_step, in_coef, out_coef, skip_gain
    )
    mixed_rows = gather_features(mixed_part, 1)

    own_rows = lambda values: lax.dynamic_slice_in_dim(values, tp_place * per_dev, per_dev, 0)
    own_after = own_rows(full_resid) + jnp.dot(
        own_rows(mixed_rows), out_weight, preferred_element_type=jnp.float32
    )
    own_mid = layer_norm(own_after, mid_gain).astype(jnp.bfloat16)
    weights = route_weight / jnp.sum(route_weight, axis=-1, keepdims=True) * routed_scale
    tail = [own_rows(routes).astype(jnp.bfloat16)] + three_terms(own_rows(weights))
    tail.append(jnp.zeros((per_dev, lanes - 4 * top_count), jnp.bfloat16))
    sent = jnp.concatenate([own_mid] + tail, axis=1)
    half = width // 2
    parts = [("zxyc", 0, half), ("zyxc", half, sent.shape[1] - half)]
    got = gather_blocks(sizes, "zxyc", parts, sent, 2).reshape(-1, sent.shape[1])

    rows = got.reshape(ep_count, seq_rows, -1)
    extra = got[:, width:].astype(jnp.float32)
    ids = extra[:, :top_count]
    parts = [extra[:, top_count * k : top_count * (k + 1)] for k in (1, 2, 3)]
    weight_of = (parts[0] + parts[1]) + parts[2]
    mine = (ep_place * tp_count + tp_place).astype(jnp.float32)
    hits = ids == mine
    hit = jnp.any(hits, axis=1).reshape(ep_count, seq_rows)
    hit_weight = jnp.sum(jnp.where(hits, weight_of, 0.0), axis=1).reshape(ep_count, seq_rows)
    places = jnp.arange(seq_rows)
    earlier = (places[:, None] < places[None, :]).astype(jnp.bfloat16)
    rank = jnp.dot(hit.astype(jnp.bfloat16), earlier, preferred_element_type=jnp.float32)
    chosen = hit[:, None, :] & (
        rank[:, None, :] == jnp.arange(capacity, dtype=jnp.float32)[None, :, None]
    )
    onehot = chosen.astype(jnp.bfloat16)
    slot_weight = jnp.sum(jnp.where(chosen, hit_weight[:, None, :], 0.0), axis=2)
    picked = jnp.einsum("gjr,grd->gjd", onehot, rows, preferred_element_type=jnp.float32)
    picked = picked.astype(jnp.bfloat16).reshape(ep_count * capacity, -1)[:, :width]

    def two_layers(values, gate_weight, up_weight, down_weight):
        gate_part = jnp.dot(values, gate_weight, preferred_element_type=jnp.float32)
        up_part = jnp.dot(values, up_weight, preferred_element_type=jnp.float32)
        hidden = (jax.nn.silu(gate_part) * up_part).astype(jnp.bfloat16)
        return jnp.dot(hidden, down_weight, preferred_element_type=jnp.float32)

    result = two_layers(picked, expert_gate[0], expert_up[0], expert_down[0])
    result = (result * slot_weight.reshape(-1)[:, None]).astype(jnp.bfloat16)
    spread = jnp.einsum(
        "gjr,gjd->grd",
        onehot,
        result.reshape(ep_count, capacity, width),
        preferred_element_type=jnp.float32,
    )
    piece = lax.dynamic_slice_in_dim(rows, tp_place * per_dev, per_dev, 1)
    piece = piece[:, :, :width].reshape(-1, width)
    gate_value = jax.nn.sigmoid(jnp.dot(piece, gate_vector, preferred_element_type=jnp.float32))
    shared = two_layers(piece, shared_gate, shared_up, shared_down) * gate_value[:, None]
    is_own = (jnp.arange(tp_count) == tp_place)[None, :, None, None]
    total = spread.reshape(ep_count, tp_count, per_dev, width) + jnp.where(
        is_own, shared.reshape(ep_count, 1, per_dev, width), 0.0
    )
    total = total.astype(jnp.bfloat16).reshape(-1, per_dev, width)
    parts = [("cyxz", 0, half), ("cxyz", half, half)]
    layer_out = scatter_blocks(sizes, "zxyc", parts, total, own_after, 3)
    return (layer_out, new_state)


def solution(mesh):
    return jax.shard_map(
        per_device,
        mesh=mesh,
        in_specs=(
            P("ep", "tp"),
            P(),
            P(None, "tp"),
            P(None, "ep", "tp"),
            P("tp", None),
            P("tp", None),
            P("tp"),
            P(None, "tp", None, None),
            P(None, "tp", None, None),
            P("tp"),
            P(),
            P(),
            P(),
            P("ep", None),
            P("ep", None),
            P(("ep", "tp"), None, None),
            P(("ep", "tp"), None, None),
            P(("ep", "tp"), None, None),
            P(None, "ep"),
            P(None, "ep"),
            P("ep", None),
        ),
        out_specs=(P(("ep", "tp"), None), P(None, "ep", "tp")),
        check_vma=False,
    )
```
